128 devices in a mesh: rep: 4 (over z), fs: 4 (over y), tp: 8 (over x, core).
Axes of the slice: x: 4, y: 4, z: 4, core: 2. Of those that a mesh axis runs over, the one named last changes fastest.
Arguments:
- tokens_in: bfloat16 [12288, 1024], P(('rep', 'fs', 'tp')), may hold values from -6 to 6
- out_grad: bfloat16 [12288, 1024], P(('rep', 'fs', 'tp')), may hold values from -24 to 24
- gate_weight: bfloat16 [1024, 2816], P('fs', 'tp'), may hold values from -0.1875 to 0.1875
- up_weight: bfloat16 [1024, 2816], P('fs', 'tp'), may hold values from -0.1875 to 0.1875
- down_weight: bfloat16 [2816, 1024], P('tp', 'fs'), may hold values from -0.109375 to 0.109375
Outputs:
- grad_in: bfloat16 [12288, 1024], P(('rep', 'fs', 'tp'))
- grad_gate_w: float32 [1024, 2816], P('fs', 'tp')
- grad_up_w: float32 [1024, 2816], P('fs', 'tp')
- grad_down_w: float32 [2816, 1024], P('tp', 'fs')
The draws below stay inside these ranges and needn't reach their ends.
All inputs are finite; a program needn't handle non-finite values.
Results may differ from the reference program's by a relative error of at most 0.02.
Values may be sent and summed in bfloat16 or wider, within the bound.
No kernel may reach another device: no remote copies, remote signals or barrier semaphores. Data moves between devices by JAX's collectives and lax.ppermute only.
A program may use at most 64 MiB of HBM per device.

```python
import jax
import jax.numpy as jnp

D = 1024
FF = 2816
TOKENS = 12288


def raised(result, rng, source, target, shards_of, factor):
    def block_of(dim):
        return (jnp.arange(result.shape[dim]) // (result.shape[dim] // shards_of)).reshape((-1,) + (1,) * (result.ndim - 1 - dim))

    first = jax.random.permutation(rng, shards_of)[block_of(target)]
    other_side = (block_of(target) + shards_of // 2) % shards_of
    return jnp.where((block_of(source) == first) | (block_of(source) == other_side), factor * result, result)


def steps_of(stream_key, shape, cuts, least, largest):
    factor_of = 1.0
    for axis_at, parts in cuts:
        heights = jax.random.uniform(jax.random.fold_in(jax.random.fold_in(stream_key, 6), axis_at), (parts,), jnp.float32, least / len(cuts), largest / len(cuts))
        factor_of = factor_of * jnp.repeat(jnp.exp(heights), shape[axis_at] // parts).reshape((-1,) + (1,) * (len(shape) - 1 - axis_at))
    return factor_of


def bell_draw(stream_key, dims, scale, limit, pieces=(), dtype=jnp.bfloat16):
    entries = scale * jax.random.normal(stream_key, dims, jnp.float32)
    if pieces:
        entries = entries * steps_of(stream_key, dims, pieces, -0.22, 0.18)
    return jnp.clip(entries, -limit, limit).astype(dtype)


def noise_with(stream_key, extent, deviation, limit, split, heavy, dtype=jnp.bfloat16):
    values = deviation * jax.random.normal(stream_key, extent, jnp.float32)
    if split:
        values = values * steps_of(stream_key, extent, split, -0.22, 0.18)
    return jnp.clip(raised(values, jax.random.fold_in(stream_key, 3), *heavy), -limit, limit).astype(dtype)


def setup_inputs(seed: int = 0) -> dict:
    arg_keys = jax.random.split(jax.random.key(seed), 6)
    tokens_in = bell_draw(arg_keys[0], (TOKENS, D), 1.0, 6.0, ((0, 128),))
    out_grad = noise_with(arg_keys[1], (TOKENS, D), 1.0, 24.0, ((0, 128),), (0, 1, 128, 5.5))
    gate_weight = bell_draw(arg_keys[2], (D, FF), D ** -0.5, 0.1875, ((0, 4), (1, 8)))
    up_weight = bell_draw(arg_keys[3], (D, FF), D ** -0.5, 0.1875, ((0, 4), (1, 8)))
    down_weight = bell_draw(arg_keys[4], (FF, D), FF ** -0.5, 0.109375, ((0, 8), (1, 4)))
    return dict(tokens_in=tokens_in, out_grad=out_grad, gate_weight=gate_weight, up_weight=up_weight, down_weight=down_weight)


def reference(tokens_in, out_grad, gate_weight, up_weight, down_weight):
    gate = jnp.dot(tokens_in, gate_weight, preferred_element_type=jnp.float32).astype(jnp.bfloat16)
    up_proj = jnp.dot(tokens_in, up_weight, preferred_element_type=jnp.float32).astype(jnp.bfloat16)
    gate_wide = gate.astype(jnp.float32)
    up_wide = up_proj.astype(jnp.float32)
    sigmoid = jax.nn.sigmoid(gate_wide)
    activated = gate_wide * sigmoid
    hidden = (activated * up_wide).astype(jnp.bfloat16)
    grad_hidden = jnp.dot(out_grad, down_weight.T, preferred_element_type=jnp.float32).astype(jnp.bfloat16)
    grad_wide = grad_hidden.astype(jnp.float32)
    grad_gate = (grad_wide * up_wide * sigmoid * (1.0 + gate_wide * (1.0 - sigmoid))).astype(jnp.bfloat16)
    grad_up = (grad_wide * activated).astype(jnp.bfloat16)
    grad_in = (jnp.dot(grad_gate, gate_weight.T, preferred_element_type=jnp.float32)
               + jnp.dot(grad_up, up_weight.T, preferred_element_type=jnp.float32)).astype(jnp.bfloat16)
    factor = TOKENS ** -0.5
    grad_gate_w = jnp.dot(tokens_in.T, grad_gate, preferred_element_type=jnp.float32) * factor
    grad_up_w = jnp.dot(tokens_in.T, grad_up, preferred_element_type=jnp.float32) * factor
    grad_down_w = jnp.dot(hidden.T, out_grad, preferred_element_type=jnp.float32) * factor
    return grad_in, grad_gate_w, grad_up_w, grad_down_w
```

```python
import jax
import jax.numpy as jnp
from jax import lax
from jax.experimental import pallas as pl
from jax.experimental.pallas import tpu as pltpu
from jax.sharding import Mesh, PartitionSpec as P


BF = jnp.bfloat16
F32 = jnp.float32


def nt(a, b):
    return lax.dot_general(a, b, (((1,), (1,)), ((), ())), preferred_element_type=F32)


def nn(a, b):
    return lax.dot_general(a, b, (((1,), (0,)), ((), ())), preferred_element_type=F32)


def tn(a, b):
    return lax.dot_general(a, b, (((0,), (0,)), ((), ())), preferred_element_type=F32)


def block(index, width):
    return pl.ds(pl.multiple_of(index * width, width), width)


def pack_kernel(x, g, wg, wu, wd, xg, w):
    rows = x.shape[0]
    hid = wg.shape[0]
    half = hid // 2
    xg[:rows] = x[...]
    xg[rows:] = g[...]
    w[:hid] = wg[...]
    w[hid : hid + half] = wd[:half]
    w[hid + half : 2 * hid] = wd[half:]
    w[2 * hid :] = wu[...]


def forward_kernel(factor, *refs):
    blocks = refs[:8]
    own, right, left, far_r, far_l = refs[8:13]
    xs, gs, gate_t, up_t, wg, wu, wd, d0, d1, d2, d3 = refs[13:]
    rows = blocks[0].shape[0] // 2
    hid, width = wg.shape[0], own.shape[1]
    f = lax.axis_index("fs")
    for i, b in enumerate(blocks):
        xs[i * rows : (i + 1) * rows] = b[:rows]
        gs[i * rows : (i + 1) * rows] = b[rows:]
    for ref, shift in ((own, 0), (right, 3), (left, 1)):
        cols = block((f + shift) % 4, width)
        wg[:, cols] = ref[:hid]
        wd[:, cols] = ref[hid : 2 * hid]
        wu[:, cols] = ref[2 * hid :]
    cols = block((f + 2) % 4, width)
    half = hid // 2
    wg[:, cols] = far_r[:hid]
    wd[:half, cols] = far_r[hid:]
    wd[half:, cols] = far_l[:half]
    wu[:, cols] = far_l[half:]
    gate = nt(wg[...], xs[...]).astype(BF)
    up = nt(wu[...], xs[...]).astype(BF)
    gate_t[...] = gate
    up_t[...] = up
    wide = gate.astype(F32)
    hidden = (wide * jax.nn.sigmoid(wide) * up.astype(F32)).astype(BF)
    for k, out in enumerate((d0, d1, d2, d3)):
        out[...] = (factor * nn(hidden, gs[:, block((f + k) % 4, width)])).astype(BF)


def backward_kernel(factor, xs, gs, gate_t, up_t, wd, gg_t, gu_t, a0, a1, a2, a3, b0, b1, b2, b3):
    width = a0.shape[1]
    f = lax.axis_index("fs")
    grad = nt(wd[...], gs[...]).astype(BF).astype(F32)
    gate = gate_t[...].astype(F32)
    up = up_t[...].astype(F32)
    sig = jax.nn.sigmoid(gate)
    grad_gate = (grad * up * sig * (1.0 + gate * (1.0 - sig))).astype(BF)
    grad_up = (grad * (gate * sig)).astype(BF)
    gg_t[...] = grad_gate
    gu_t[...] = grad_up
    for k, (a, b) in enumerate(((a0, b0), (a1, b1), (a2, b2), (a3, b3))):
        cols = xs[:, block((f + k) % 4, width)]
        a[...] = (factor * nn(grad_gate, cols)).astype(BF)
        b[...] = (factor * nn(grad_up, cols)).astype(BF)


def input_kernel(gg_t, gu_t, wg, wu, mine, other):
    half = mine.shape[0]
    mine[...] = tn(gg_t[:, :half], wg[...]) + tn(gu_t[:, :half], wu[...])
    other[...] = (tn(gg_t[:, half:], wg[...]) + tn(gu_t[:, half:], wu[...])).astype(BF)


def call(kernel, outs, *args):
    spec = pl.BlockSpec(memory_space=pltpu.VMEM)
    return pl.pallas_call(
        kernel,
        out_shape=[jax.ShapeDtypeStruct(*o) for o in outs],
        in_specs=[spec] * len(args),
        out_specs=[spec] * len(outs),
        compiler_params=pltpu.CompilerParams(vmem_limit_bytes=60 * 2**20),
    )(*args)


def ring(k):
    return [(i, (i + k) % 4) for i in range(4)]


def along(axis, value, k):
    return lax.ppermute(value, axis, ring(k))


def swap(value):
    return lax.ppermute(value, "tc", [(0, 1), (1, 0)])


def total(own, others):
    one, two, three = (o.astype(F32) for o in others)
    return (own.astype(F32) + two) + (one + three)


def body(tokens_in, out_grad, gate_weight, up_weight, down_weight):
    rows, model = tokens_in.shape
    width, hid = gate_weight.shape
    toks = 8 * rows
    factor = (toks * 16) ** (-0.5)
    xg, w = call(
        pack_kernel,
        [((2 * rows, model), BF), ((3 * hid, width), BF)],
        tokens_in,
        out_grad,
        gate_weight.T,
        up_weight.T,
        down_weight,
    )
    cut = hid + hid // 2
    right = along("fs", w, 1)
    left = along("fs", w, 3)
    got = [along("tx", xg, k) for k in (1, 3, 2)]
    far_r = along("fs", right[:cut], 1)
    far_l = along("fs", left[cut:], 3)
    mine = [xg, got[0], got[2], got[1]]
    blocks = mine + [swap(b) for b in mine]
    big = ((toks, model), BF)
    hidden_shape = ((hid, toks), BF)
    weight = ((hid, model), BF)
    part = ((hid, width), BF)
    xs, gs, gate_t, up_t, wg, wu, wd, *downs = call(
        lambda *r: forward_kernel(factor, *r),
        [big, big, hidden_shape, hidden_shape, weight, weight, weight] + [part] * 4,
        *blocks,
        w,
        right,
        left,
        far_r,
        far_l,
    )

    def scattered(parts):
        return total(parts[0], [along("fs", parts[k], k) for k in (1, 2, 3)]).astype(BF)

    def replicated(value):
        return total(value, [along("rep", value, k) for k in (1, 2, 3)])

    down = scattered(downs)
    gg_t, gu_t, *parts = call(
        lambda *r: backward_kernel(factor, *r),
        [hidden_shape, hidden_shape] + [part] * 8,
        xs,
        gs,
        gate_t,
        up_t,
        wd,
    )
    gate = scattered(parts[:4])
    up = scattered(parts[4:])
    kept, given = call(
        input_kernel, [((toks // 2, model), F32), ((toks // 2, model), BF)], gg_t, gu_t, wg, wu
    )
    pairs = kept + swap(given).astype(F32)
    pieces = [pairs[k * rows : (k + 1) * rows].astype(BF) for k in range(4)]
    grad_in = total(pieces[0], [along("tx", pieces[k], -k) for k in (1, 2, 3)]).astype(BF)
    down, gate, up = replicated(down), replicated(gate), replicated(up)
    return (grad_in, gate.T, up.T, down)


def solution(mesh):
    split = Mesh(mesh.devices.reshape(4, 4, 4, 2), ("rep", "fs", "tx", "tc"))
    tokens = P(("rep", "fs", "tx", "tc"), None)
    columns = P("fs", ("tx", "tc"))
    lines = P(("tx", "tc"), "fs")
    return jax.shard_map(
        body,
        mesh=split,
        in_specs=(tokens, tokens, columns, columns, lines),
        out_specs=(tokens, columns, columns, lines),
        check_vma=False,
    )
```

```python
import jax
import jax.numpy as jnp
from jax import lax
from jax.experimental import pallas as pl
from jax.experimental.pallas import tpu as pltpu
from jax.sharding import Mesh, PartitionSpec as P


BF = jnp.bfloat16
F32 = jnp.float32

UP = [(2 * i + c, 2 * ((i + (1, 3)[c]) % 4) + c) for i in range(4) for c in range(2)]
DOWN = [(b, a) for a, b in UP]
PAIRS = [(2 * i + c, 2 * ((i ^ 1, 3 - i)[c]) + c) for i in range(4) for c in range(2)]
CROSS = [(2 * i + c, 2 * ((3 - i, i ^ 1)[c]) + c) for i in range(4) for c in range(2)]
SWAP = [(0, 1), (1, 0)]


def nt(a, b):
    return lax.dot_general(a, b, (((1,), (1,)), ((), ())), preferred_element_type=F32)


def nn(a, b):
    return lax.dot_general(a, b, (((1,), (0,)), ((), ())), preferred_element_type=F32)


def tn(a, b):
    return lax.dot_general(a, b, (((0,), (0,)), ((), ())), preferred_element_type=F32)


def columns_of(width):
    f = lax.axis_index("fs")
    step = 1 - 2 * lax.axis_index("tc")
    return [
        pl.ds(pl.multiple_of(((f + d) % 4) * width, width), width)
        for d in (0, 4 - step, 4 + step, 2)
    ]


def pack_kernel(x, g, wg, wu, wd, xg, w, sems):
    rows, hid = x.shape[0], wg.shape[0]
    places = (
        (wg, w.at[:hid]),
        (wu, w.at[hid : 2 * hid]),
        (wd, w.at[2 * hid :]),
        (x, xg.at[:rows]),
        (g, xg.at[rows:]),
    )
    copies = [pltpu.make_async_copy(a, b, sems.at[i]) for i, (a, b) in enumerate(places)]
    for copy in copies:
        copy.start()
    for copy in copies:
        copy.wait()


def forward_kernel(factor, *refs):
    blocks, weights = refs[:8], refs[8:12]
    xs, gs, gate_t, up_t, wg, wu, wd, own, behind, ahead, far = refs[12:]
    rows = blocks[0].shape[0] // 2
    hid, width = own.shape
    places = columns_of(width)
    for i, b in enumerate(blocks):
        xs[i * rows : (i + 1) * rows] = b[:rows]
        gs[i * rows : (i + 1) * rows] = b[rows:]
    for ref, cols in zip(weights, places):
        wg[:, cols] = ref[:hid]
        wu[:, cols] = ref[hid : 2 * hid]
        wd[:, cols] = ref[2 * hid :]
    gate = nt(wg[...], xs[...]).astype(BF)
    up = nt(wu[...], xs[...]).astype(BF)
    gate_t[...] = gate
    up_t[...] = up
    wide = gate.astype(F32)
    hidden = (wide * jax.nn.sigmoid(wide) * up.astype(F32)).astype(BF)
    for out, cols in zip((own, behind, ahead, far), places):
        out[...] = (factor * nn(hidden, gs[:, cols])).astype(BF)


def backward_kernel(factor, xs, gs, gate_t, up_t, wd, gg_t, gu_t, *outs):
    hid = wd.shape[0]
    grad = nt(wd[...], gs[...]).astype(BF).astype(F32)
    gate = gate_t[...].astype(F32)
    up = up_t[...].astype(F32)
    sig = jax.nn.sigmoid(gate)
    grad_gate = (grad * up * sig * (1.0 + gate * (1.0 - sig))).astype(BF)
    grad_up = (grad * (gate * sig)).astype(BF)
    gg_t[...] = grad_gate
    gu_t[...] = grad_up
    for out, cols in zip(outs, columns_of(outs[0].shape[1])):
        x = xs[:, cols]
        out[:hid] = (factor * nn(grad_gate, x)).astype(BF)
        out[hid:] = (factor * nn(grad_up, x)).astype(BF)


def input_kernel(gg_t, gu_t, wg, wu, mine, other):
    half = mine.shape[0]
    mine[...] = tn(gg_t[:, :half], wg[...]) + tn(gu_t[:, :half], wu[...])
    other[...] = (tn(gg_t[:, half:], wg[...]) + tn(gu_t[:, half:], wu[...])).astype(BF)


def pair_kernel(mine, other, own, behind, far, ahead):
    rows = own.shape[0]
    for i, out in enumerate((own, behind, far, ahead)):
        part = slice(i * rows, (i + 1) * rows)
        out[...] = (mine[part] + other[part].astype(F32)).astype(out.dtype)


def outputs_kernel(own, behind, ahead, down_a, down_b, grad_in, down):
    grad_in[...] = (own[...] + behind[...].astype(F32) + ahead[...].astype(F32)).astype(BF)
    down[...] = down_a[...].astype(F32) + down_b[...].astype(F32)


def weights_kernel(a, b, gate, up):
    hid = gate.shape[0]
    gate[...] = a[:hid].astype(F32) + b[:hid].astype(F32)
    up[...] = a[hid:].astype(F32) + b[hid:].astype(F32)


def call(kernel, outs, *args, inputs=pltpu.VMEM, outputs=pltpu.VMEM, scratch=()):
    inside = pl.BlockSpec(memory_space=pltpu.VMEM)
    given = pl.BlockSpec(memory_space=inputs)
    args = [pltpu.with_memory_space_constraint(a, inputs) for a in args]
    return pl.pallas_call(
        kernel,
        out_shape=[outputs(*o) if outputs else jax.ShapeDtypeStruct(*o) for o in outs],
        in_specs=[given] * len(args),
        out_specs=[inside] * len(outs),
        scratch_shapes=list(scratch),
        compiler_params=pltpu.CompilerParams(vmem_limit_bytes=16 * 2**20),
    )(*args)


def swap(value):
    return lax.ppermute(value, "tc", SWAP)


def plus(a, b):
    return (a.astype(F32) + b.astype(F32)).astype(BF)


def body(tokens_in, out_grad, gate_weight, up_weight, down_weight):
    rows, model = tokens_in.shape
    width, hid = gate_weight.shape
    toks = 8 * rows
    factor = (toks * 16) ** (-0.5)
    x_axis, y_axis, z_axis = ("tx", "tc"), ("fs", "tc"), ("rep", "tc")
    xg, w = call(
        pack_kernel,
        [((2 * rows, model), BF), ((3 * hid, width), BF)],
        tokens_in,
        out_grad,
        gate_weight.T,
        up_weight.T,
        down_weight,
        inputs=pltpu.HBM,
        scratch=[pltpu.SemaphoreType.DMA((5,))],
    )
    w_behind = lax.ppermute(w, y_axis, UP)
    x_behind = lax.ppermute(xg, x_axis, UP)
    w_other, x_other = swap(w), swap(xg)
    w_second = lax.ppermute(w_other, y_axis, UP)
    x_second = lax.ppermute(x_other, x_axis, UP)
    w_far = lax.ppermute(w_behind, y_axis, UP)
    x_far = lax.ppermute(x_behind, x_axis, UP)
    w_ahead = swap(w_second)
    blocks = [xg, x_behind, x_far, swap(x_second), x_other, swap(x_behind), swap(x_far), x_second]
    big = ((toks, model), BF)
    hidden_shape = ((hid, toks), BF)
    weight = ((hid, model), BF)
    xs, gs, gate_t, up_t, wg, wu, wd, *downs = call(
        lambda *r: forward_kernel(factor, *r),
        [big, big, hidden_shape, hidden_shape, weight, weight, weight] + [((hid, width), BF)] * 4,
        *blocks,
        w,
        w_behind,
        w_ahead,
        w_far,
    )

    def scattered(axes, own, behind, ahead, far):
        relayed = lax.ppermute(far, axes, UP)
        back = lax.ppermute(behind, axes, DOWN)
        front = lax.ppermute(plus(ahead, relayed), axes, UP)
        return own, back, front

    def reduced(own, back, front):
        part = (own.astype(F32) + back.astype(F32) + front.astype(F32)).astype(BF)
        pair = plus(part, lax.ppermute(part, z_axis, PAIRS))
        return pair, lax.ppermute(pair, z_axis, CROSS)

    down = reduced(*scattered(y_axis, *downs))
    gg_t, gu_t, *parts = call(
        lambda *r: backward_kernel(factor, *r),
        [hidden_shape, hidden_shape] + [((2 * hid, width), BF)] * 4,
        xs,
        gs,
        gate_t,
        up_t,
        wd,
    )
    both = reduced(*scattered(y_axis, *parts))
    half = ((toks // 2, model),)
    kept, given = call(input_kernel, [half + (F32,), half + (BF,)], gg_t, gu_t, wg, wu)
    piece = (rows, model)
    own, behind, far, ahead = call(
        pair_kernel, [(piece, F32)] + [(piece, BF)] * 3, kept, swap(given)
    )
    grad_parts = scattered(x_axis, own, behind, ahead, far)
    grad_in, grad_down = call(
        outputs_kernel, [(piece, BF), ((hid, width), F32)], *grad_parts, *down, outputs=None
    )
    grad_gate, grad_up = call(weights_kernel, [((hid, width), F32)] * 2, *both, outputs=None)
    return (grad_in, grad_gate.T, grad_up.T, grad_down)


def solution(mesh):
    split = Mesh(mesh.devices.reshape(4, 4, 4, 2), ("rep", "fs", "tx", "tc"))
    tokens = P(("rep", "fs", "tx", "tc"), None)
    columns = P("fs", ("tx", "tc"))
    lines = P(("tx", "tc"), "fs")
    return jax.shard_map(
        body,
        mesh=split,
        in_specs=(tokens, tokens, columns, columns, lines),
        out_specs=(tokens, columns, columns, lines),
        check_vma=False,
    )
```

```python
import jax
import jax.numpy as jnp
from jax import lax
from jax.experimental import pallas as pl
from jax.experimental.pallas import tpu as pltpu
from jax.sharding import Mesh, PartitionSpec as P


BF = jnp.bfloat16
F32 = jnp.float32

UP = [(2 * i + c, 2 * ((i + (1, 3)[c]) % 4) + c) for i in range(4) for c in range(2)]
DOWN = [(b, a) for a, b in UP]
PAIRS = [(2 * i + c, 2 * ((i ^ 1, 3 - i)[c]) + c) for i in range(4) for c in range(2)]
CROSS = [(2 * i + c, 2 * ((3 - i, i ^ 1)[c]) + c) for i in range(4) for c in range(2)]
SWAP = [(0, 1), (1, 0)]


def nt(a, b):
    return lax.dot_general(a, b, (((1,), (1,)), ((), ())), preferred_element_type=F32)


def nn(a, b):
    return lax.dot_general(a, b, (((1,), (0,)), ((), ())), preferred_element_type=F32)


def tn(a, b):
    return lax.dot_general(a, b, (((0,), (0,)), ((), ())), preferred_element_type=F32)


def columns_of(width):
    f = lax.axis_index("fs")
    step = 1 - 2 * lax.axis_index("tc")
    return [
        pl.ds(pl.multiple_of(((f + d) % 4) * width, width), width)
        for d in (0, 4 - step, 4 + step, 2)
    ]


def pack_kernel(x, g, wg, wu, wd, xg, w, d, sems):
    rows, hid = x.shape[0], wg.shape[0]
    places = (
        (x, xg.at[:rows]),
        (g, xg.at[rows:]),
        (wg, w.at[:hid]),
        (wu, w.at[hid:]),
        (wd, d),
    )
    copies = [pltpu.make_async_copy(a, b, sems.at[i]) for i, (a, b) in enumerate(places)]
    for copy in copies:
        copy.start()
    for copy in copies:
        copy.wait()


def forward_kernel(factor, *refs):
    blocks, weights = refs[:8], refs[8:12]
    xs, gs, gate_t, up_t, wg, wu, own, behind, ahead, far = refs[12:]
    rows = blocks[0].shape[0] // 2
    hid, width = own.shape
    places = columns_of(width)
    for i, b in enumerate(blocks):
        xs[i * rows : (i + 1) * rows] = b[:rows]
        gs[i * rows : (i + 1) * rows] = b[rows:]
    for ref, cols in zip(weights, places):
        wg[:, cols] = ref[:hid]
        wu[:, cols] = ref[hid:]
    gate = nt(wg[...], xs[...]).astype(BF)
    up = nt(wu[...], xs[...]).astype(BF)
    gate_t[...] = gate
    up_t[...] = up
    wide = gate.astype(F32)
    hidden = (wide * jax.nn.sigmoid(wide) * up.astype(F32)).astype(BF)
    for out, cols in zip((own, behind, ahead, far), places):
        out[...] = (factor * nn(hidden, gs[:, cols])).astype(BF)


def backward_kernel(factor, xs, gs, gate_t, up_t, *refs):
    weights, (gg_t, gu_t), outs, wd = refs[:4], refs[4:6], refs[6:10], refs[10]
    hid, width = weights[0].shape
    places = columns_of(width)
    for ref, cols in zip(weights, places):
        wd[:, cols] = ref[...]
    grad = nt(wd[...], gs[...]).astype(BF).astype(F32)
    gate = gate_t[...].astype(F32)
    up = up_t[...].astype(F32)
    sig = jax.nn.sigmoid(gate)
    grad_gate = (grad * up * sig * (1.0 + gate * (1.0 - sig))).astype(BF)
    grad_up = (grad * (gate * sig)).astype(BF)
    gg_t[...] = grad_gate
    gu_t[...] = grad_up
    for out, cols in zip(outs, places):
        x = xs[:, cols]
        out[:hid] = (factor * nn(grad_gate, x)).astype(BF)
        out[hid:] = (factor * nn(grad_up, x)).astype(BF)


def input_kernel(gg_t, gu_t, wg, wu, mine, other):
    half = mine.shape[0]
    mine[...] = tn(gg_t[:, :half], wg[...]) + tn(gu_t[:, :half], wu[...])
    other[...] = (tn(gg_t[:, half:], wg[...]) + tn(gu_t[:, half:], wu[...])).astype(BF)


def pair_kernel(mine, other, own, behind, far, ahead):
    rows = own.shape[0]
    for i, out in enumerate((own, behind, far, ahead)):
        part = slice(i * rows, (i + 1) * rows)
        out[...] = (mine[part] + other[part].astype(F32)).astype(out.dtype)


def grad_kernel(own, behind, ahead, grad_in):
    grad_in[...] = (own[...] + behind[...].astype(F32) + ahead[...].astype(F32)).astype(BF)


def weights_kernel(a, b, down_a, down_b, gate, up, down):
    hid = gate.shape[0]
    gate[...] = a[:hid].astype(F32) + b[:hid].astype(F32)
    up[...] = a[hid:].astype(F32) + b[hid:].astype(F32)
    down[...] = down_a[...].astype(F32) + down_b[...].astype(F32)


def call(kernel, outs, *args, inputs=pltpu.VMEM, outputs=pltpu.VMEM, scratch=()):
    inside = pl.BlockSpec(memory_space=pltpu.VMEM)
    given = pl.BlockSpec(memory_space=inputs)
    args = [pltpu.with_memory_space_constraint(a, inputs) for a in args]
    return pl.pallas_call(
        kernel,
        out_shape=[outputs(*o) if outputs else jax.ShapeDtypeStruct(*o) for o in outs],
        in_specs=[given] * len(args),
        out_specs=[inside] * len(outs),
        scratch_shapes=list(scratch),
        compiler_params=pltpu.CompilerParams(vmem_limit_bytes=16 * 2**20),
    )(*args)


def swap(value):
    return lax.ppermute(value, "tc", SWAP)


def plus(a, b):
    return (a.astype(F32) + b.astype(F32)).astype(BF)


def body(tokens_in, out_grad, gate_weight, up_weight, down_weight):
    rows, model = tokens_in.shape
    width, hid = gate_weight.shape
    toks = 8 * rows
    factor = (toks * 16) ** (-0.5)
    x_axis, y_axis, z_axis = ("tx", "tc"), ("fs", "tc"), ("rep", "tc")
    xg, w, d = call(
        pack_kernel,
        [((2 * rows, model), BF), ((2 * hid, width), BF), ((hid, width), BF)],
        tokens_in,
        out_grad,
        gate_weight.T,
        up_weight.T,
        down_weight,
        inputs=pltpu.HBM,
        scratch=[pltpu.SemaphoreType.DMA((5,))],
    )

    def gathered(axes, value):
        behind = lax.ppermute(value, axes, UP)
        other = swap(value)
        second = lax.ppermute(other, axes, UP)
        return other, behind, second, lax.ppermute(behind, axes, UP)

    x_other, x_behind, x_second, x_far = gathered(x_axis, xg)
    _, w_behind, w_second, w_far = gathered(y_axis, w)
    _, d_behind, d_second, d_far = gathered(y_axis, d)
    blocks = [xg, x_behind, x_far, swap(x_second), x_other, swap(x_behind), swap(x_far), x_second]
    big = ((toks, model), BF)
    hidden_shape = ((hid, toks), BF)
    weight = ((hid, model), BF)
    xs, gs, gate_t, up_t, wg, wu, *downs = call(
        lambda *r: forward_kernel(factor, *r),
        [big, big, hidden_shape, hidden_shape, weight, weight] + [((hid, width), BF)] * 4,
        *blocks,
        w,
        w_behind,
        swap(w_second),
        w_far,
    )

    def scattered(axes, own, behind, ahead, far):
        relayed = lax.ppermute(far, axes, UP)
        back = lax.ppermute(behind, axes, DOWN)
        front = lax.ppermute(plus(ahead, relayed), axes, UP)
        return own, back, front

    def reduced(own, back, front):
        part = (own.astype(F32) + back.astype(F32) + front.astype(F32)).astype(BF)
        pair = plus(part, lax.ppermute(part, z_axis, PAIRS))
        return pair, lax.ppermute(pair, z_axis, CROSS)

    down = reduced(*scattered(y_axis, *downs))
    gg_t, gu_t, *parts = call(
        lambda *r: backward_kernel(factor, *r),
        [hidden_shape, hidden_shape] + [((2 * hid, width), BF)] * 4,
        xs,
        gs,
        gate_t,
        up_t,
        d,
        d_behind,
        swap(d_second),
        d_far,
        scratch=[pltpu.VMEM((hid, model), BF)],
    )
    both = reduced(*scattered(y_axis, *parts))
    half = ((toks // 2, model),)
    kept, given = call(input_kernel, [half + (F32,), half + (BF,)], gg_t, gu_t, wg, wu)
    piece = (rows, model)
    own, behind, far, ahead = call(
        pair_kernel, [(piece, F32)] + [(piece, BF)] * 3, kept, swap(given)
    )
    grad_parts = scattered(x_axis, own, behind, ahead, far)
    (grad_in,) = call(grad_kernel, [(piece, BF)], *grad_parts, outputs=None)
    grad_gate, grad_up, grad_down = call(
        weights_kernel, [((hid, width), F32)] * 3, *both, *down, outputs=None
    )
    return (grad_in, grad_gate.T, grad_up.T, grad_down)


def solution(mesh):
    split = Mesh(mesh.devices.reshape(4, 4, 4, 2), ("rep", "fs", "tx", "tc"))
    tokens = P(("rep", "fs", "tx", "tc"), None)
    columns = P("fs", ("tx", "tc"))
    lines = P(("tx", "tc"), "fs")
    return jax.shard_map(
        body,
        mesh=split,
        in_specs=(tokens, tokens, columns, columns, lines),
        out_specs=(tokens, columns, columns, lines),
        check_vma=False,
    )
```
